32 devices in a mesh: sp: 8 (over z, y), tp: 4 (over x, core).
Axes of the slice: x: 2, y: 2, z: 4, core: 2. Of those that a mesh axis runs over, the one named last changes fastest.
Arguments:
- tokens: bfloat16 [3072, 4096], P(('sp', 'tp')), may hold values from -6 to 6
- norm_gain: float32 [4096], replicated, may hold values from 0.1 to 1.9
- w_query: bfloat16 [4096, 2048], P('sp', 'tp'), may hold values from -0.09375 to 0.09375
- w_key: bfloat16 [4096, 512], P('sp', 'tp'), may hold values from -1.5 to 1.5
- w_value: bfloat16 [4096, 512], P('sp', 'tp'), may hold values from -0.09375 to 0.09375
- w_mem_query: bfloat16 [4096, 1024], P('sp', 'tp'), may hold values from -0.09375 to 0.09375
- w_mem_key: bfloat16 [4096, 1024], P('sp', 'tp'), may hold values from -0.09375 to 0.09375
- w_mem_value: bfloat16 [4096, 1024], P('sp', 'tp'), may hold values from -0.09375 to 0.09375
- w_mem_gate: bfloat16 [4096, 1024], P('sp', 'tp'), may hold values from -0.09375 to 0.09375
- w_gates: bfloat16 [4096, 2, 16], replicated, may hold values from -0.09375 to 0.09375
- sinks: float32 [32], P('tp'), may hold values from 2 to 6
- forget_bias: float32 [16], P('tp'), may hold values from 3 to 13
- forget_shift: float32 [3072, 16], P('sp', 'tp'), may hold values from -1 to 0
- w_out: bfloat16 [3072, 4096], P('sp', 'tp'), may hold values from -0.21650635 to 0.21650635
Outputs:
- mixed: bfloat16 [3072, 4096], P('sp', 'tp')
- log_total: float32 [3072, 32], P('sp', 'tp')
The draws below stay inside these ranges and needn't reach their ends.
All inputs are finite; a program needn't handle non-finite values.
Results may differ from the reference program's by a relative error of at most 0.018.
Values may be sent and summed in bfloat16 or wider, within the bound.
A program may use at most 128 MiB of HBM per device.

```python
import math
import jax
import jax.numpy as jnp
from jax import lax

D = 4096
QH = 32
KVH = 8
CELL_SUBSPACES = 16
HD = 64
WINDOW = 128
BLK = 128
TOK_DEV = 384
ITEM_COUNT = 3072
MIX = 3072


def query_base(key):
    normal_noise = jax.random.normal(jax.random.fold_in(key, 101), (D, QH * HD), jnp.float32)
    return jnp.clip(normal_noise, -6.0, 6.0) * D ** (-0.5)


def draw_w_query(key, part):
    return query_base(key).astype(jnp.bfloat16)


def draw_w_key(key, part):
    normal_noise = jax.random.normal(jax.random.fold_in(key, 102), (D, KVH * HD), jnp.float32)
    own_columns = jnp.clip(normal_noise, -6.0, 6.0) * D ** (-0.5)
    return own_columns.astype(jnp.bfloat16)


def draw_forget_bias(key, part):
    ordering = jax.random.permutation(jax.random.fold_in(key, 201), CELL_SUBSPACES)
    slow_heads = ordering < CELL_SUBSPACES // 2
    jitter = jax.random.uniform(jax.random.fold_in(key, 202), (CELL_SUBSPACES,), jnp.float32, -0.3, 0.3)
    fast_values = jax.random.uniform(jax.random.fold_in(key, 203), (CELL_SUBSPACES,), jnp.float32, 3.4, 4.6)
    slow_values = math.log(4.0 * ITEM_COUNT) + jitter
    return jnp.where(slow_heads, slow_values, fast_values).astype(jnp.float32)


def draw_forget_shift(key, part):
    device_count = ITEM_COUNT // TOK_DEV
    spread = jax.random.uniform(jax.random.fold_in(key, 301), (device_count,), jnp.float32, math.log(0.35), math.log(2.8))
    rates = jnp.exp(spread) * (-0.3 / ITEM_COUNT)
    per_element = jnp.repeat(rates, TOK_DEV, total_repeat_length=ITEM_COUNT)
    place_indices = jax.random.randint(jax.random.fold_in(key, 302), (3, CELL_SUBSPACES), 0, ITEM_COUNT)
    stack_tiers = jax.random.uniform(jax.random.fold_in(key, 303), (3, CELL_SUBSPACES), jnp.float32, 0.22, 0.69)
    element_tally = jnp.arange(ITEM_COUNT)[:, None]
    spurt_bundles = jnp.zeros((ITEM_COUNT, CELL_SUBSPACES), jnp.float32)
    for spurt_tally in range(3):
        spurt_bundles = spurt_bundles + jnp.where(element_tally == place_indices[spurt_tally][None, :], stack_tiers[spurt_tally][None, :], 0.0)
    return (per_element[:, None] - spurt_bundles).astype(jnp.float32)


def draw_w_out(key, part):
    normal_noise = jax.random.normal(jax.random.fold_in(key, 401), (MIX, D), jnp.float32)
    row_scale = jnp.where(jnp.arange(MIX) < QH * HD, 2.0, 1.0)
    return (jnp.clip(normal_noise, -6.0, 6.0) * MIX ** (-0.5) * row_scale[:, None]).astype(jnp.bfloat16)


def block_scale(stream_key, extent, pieces, smallest, high):
    gain = 1.0
    for dim, shards_of in pieces:
        draws = jax.random.uniform(jax.random.fold_in(jax.random.fold_in(stream_key, 6), dim), (shards_of,), jnp.float32, smallest / len(pieces), high / len(pieces))
        gain = gain * jnp.repeat(jnp.exp(draws), extent[dim] // shards_of).reshape((-1,) + (1,) * (len(extent) - 1 - dim))
    return gain


def noise(key, shape, scale, reach, cuts=(), held_as=jnp.bfloat16):
    values = scale * jax.random.normal(key, shape, jnp.float32)
    if cuts:
        values = values * block_scale(key, shape, cuts, -0.22, 0.18)
    return jnp.clip(values, -reach, reach).astype(held_as)


def setup_inputs(seed: int = 0) -> dict:
    key_list = jax.random.split(jax.random.key(seed), 15)
    return {
        "tokens": noise(key_list[0], (ITEM_COUNT, D), 1.0, 6.0, ((0, 32),)),
        "norm_gain": jnp.clip(1.0 + 0.18 * jax.random.normal(key_list[1], (D,), jnp.float32), 0.1, 1.9),
        "w_query": draw_w_query(jax.random.fold_in(key_list[14], 71), 0),
        "w_key": draw_w_key(jax.random.fold_in(key_list[14], 71), 0),
        "w_value": noise(key_list[4], (D, KVH * HD), D ** -0.5, 0.09375, ((0, 8), (1, 4))),
        "w_mem_query": noise(key_list[5], (D, CELL_SUBSPACES * HD), D ** -0.5, 0.09375, ((0, 8), (1, 4))),
        "w_mem_key": noise(key_list[6], (D, CELL_SUBSPACES * HD), D ** -0.5, 0.09375, ((0, 8), (1, 4))),
        "w_mem_value": noise(key_list[7], (D, CELL_SUBSPACES * HD), D ** -0.5, 0.09375, ((0, 8), (1, 4))),
        "w_mem_gate": noise(key_list[8], (D, CELL_SUBSPACES * HD), D ** -0.5, 0.09375, ((0, 8), (1, 4))),
        "w_gates": noise(key_list[9], (D, 2, CELL_SUBSPACES), D ** -0.5, 0.09375),
        "sinks": jnp.clip(2.0 + 4.0 * jax.random.uniform(key_list[10], (QH,), jnp.float32) ** block_scale(key_list[10], (QH,), ((0, 4),), -0.2, 0.2), 2.0, 6.0),
        "forget_bias": draw_forget_bias(jax.random.fold_in(key_list[14], 71), 0),
        "forget_shift": draw_forget_shift(jax.random.fold_in(key_list[14], 71), 0),
        "w_out": draw_w_out(jax.random.fold_in(key_list[14], 71), 0),
    }


EPSILON = 1e-06
MASKED = -1e+30
exact_precision = lax.Precision.HIGHEST

def normalize(tokens, norm_gain):
    values = tokens.astype(jnp.float32)
    rescale = lax.rsqrt(lax.optimization_barrier(jnp.mean(values * values, axis=-1, keepdims=True)) + EPSILON)
    return (values * rescale * norm_gain).astype(jnp.bfloat16)

def advance(carried, key_block, value_block, in_block, cumulative):
    memory_state, normalizer, stabilizer = carried
    block_total = cumulative[:, -1]
    decays = block_total[:, None] - cumulative + in_block
    new_stabilizer = jnp.maximum(block_total + stabilizer, lax.optimization_barrier(jnp.max(decays, axis=-1)))
    weights = jnp.exp(decays - new_stabilizer[:, None])
    rescale = jnp.exp(block_total + stabilizer - new_stabilizer)
    new_state = rescale[:, None, None] * memory_state + jnp.einsum('hsv,hsk->hvk', value_block * weights[:, :, None], key_block, precision=exact_precision)
    new_normalizer = rescale[:, None] * normalizer + jnp.einsum('hs,hsk->hk', weights, key_block, precision=exact_precision)
    return (new_state, new_normalizer, new_stabilizer)

def block_step(carried, block_data):
    memory_state, normalizer, stabilizer = carried
    query_block, key_block, value_block, in_block, forget_block = block_data
    length = in_block.shape[-1]
    cumulative = jnp.cumsum(forget_block, axis=-1)
    causal = lax.broadcasted_iota(jnp.int32, (length, length), 0) >= lax.broadcasted_iota(jnp.int32, (length, length), 1)
    log_weight = jnp.where(causal[None], cumulative[:, :, None] - cumulative[:, None, :] + in_block[:, None, :], MASKED)
    row_level = jnp.maximum(cumulative + stabilizer[:, None], lax.optimization_barrier(jnp.max(log_weight, axis=-1)))
    carried_part = jnp.exp(cumulative + stabilizer[:, None] - row_level)
    affinity = jnp.einsum('htd,hsd->hts', query_block, key_block, precision=exact_precision) * jnp.exp(log_weight - row_level[:, :, None])
    numerator = carried_part[:, :, None] * jnp.einsum('hvk,htk->htv', memory_state, query_block, precision=exact_precision) + jnp.einsum('hts,hsv->htv', affinity, value_block, precision=exact_precision)
    denominator = carried_part * jnp.einsum('hk,htk->ht', normalizer, query_block, precision=exact_precision) + lax.optimization_barrier(jnp.sum(affinity, axis=-1))
    recall = numerator / jnp.maximum(jnp.abs(denominator), jnp.exp(-row_level))[:, :, None]
    return (advance(carried, key_block, value_block, in_block, cumulative), recall)

def reference(tokens, norm_gain, w_query, w_key, w_value, w_mem_query, w_mem_key, w_mem_value, w_mem_gate, w_gates, sinks, forget_bias, forget_shift, w_out):
    normed = normalize(tokens, norm_gain)

    def project(weight):
        return jnp.dot(normed, weight, preferred_element_type=jnp.float32).astype(jnp.bfloat16)
    query = project(w_query)
    key_rows = project(w_key)
    value_rows = project(w_value)
    mem_query = project(w_mem_query)
    mem_key = project(w_mem_key)
    mem_value = project(w_mem_value)
    mem_gate = project(w_mem_gate)
    gate_pre = jnp.dot(normed, w_gates.reshape(D, 2 * CELL_SUBSPACES), preferred_element_type=jnp.float32).reshape(ITEM_COUNT, 2, CELL_SUBSPACES)
    group_size = QH // KVH
    block_count = ITEM_COUNT // WINDOW
    q_blocks = query.reshape(block_count, WINDOW, KVH, group_size, HD)
    zero_rim = jnp.zeros((WINDOW, KVH * HD), jnp.bfloat16)
    padded_keys = jnp.concatenate([zero_rim, key_rows], axis=0).reshape(block_count + 1, WINDOW, KVH, HD)
    padded_values = jnp.concatenate([zero_rim, value_rows], axis=0).reshape(block_count + 1, WINDOW, KVH, HD)
    key_window = jnp.concatenate([padded_keys[:-1], padded_keys[1:]], axis=1)
    value_window = jnp.concatenate([padded_values[:-1], padded_values[1:]], axis=1)
    query_index = lax.broadcasted_iota(jnp.int32, (WINDOW, 2 * WINDOW), 0)
    key_index = lax.broadcasted_iota(jnp.int32, (WINDOW, 2 * WINDOW), 1)
    distance = query_index - key_index + WINDOW
    in_band = (distance >= 0) & (distance < WINDOW)
    sink_logit = sinks.reshape(KVH, group_size, 1, 1)

    def one_block(block_data):
        query_block, key_block, value_block, block_index = block_data
        scores = jnp.einsum('qhgd,khd->hgqk', query_block.astype(jnp.float32), key_block.astype(jnp.float32)) * HD ** (-0.5)
        key_position = block_index * WINDOW - WINDOW + key_index
        allowed = in_band & (key_position >= 0)
        scores = jnp.where(allowed[None, None], scores, MASKED)
        ceiling = jnp.maximum(lax.optimization_barrier(jnp.max(scores, axis=-1, keepdims=True)), sink_logit)
        weights = jnp.exp(scores - ceiling)
        partition = jnp.exp(sink_logit - ceiling) + lax.optimization_barrier(jnp.sum(weights, axis=-1, keepdims=True))
        log_part = (ceiling + jnp.log(partition))[..., 0].transpose(2, 0, 1).reshape(WINDOW, QH)
        probs = (weights / partition).astype(jnp.bfloat16)
        head_out = jnp.einsum('hgqk,khd->qhgd', probs.astype(jnp.float32), value_block.astype(jnp.float32))
        return (head_out.astype(jnp.bfloat16).reshape(WINDOW, QH * HD), log_part)
    attn_blocks, log_blocks = lax.map(one_block, (q_blocks, key_window, value_window, jnp.arange(block_count, dtype=jnp.int32)))
    attn_out = attn_blocks.reshape(ITEM_COUNT, QH * HD)
    log_total = log_blocks.reshape(ITEM_COUNT, QH)
    log_in = gate_pre[:, 0, :] - 0.5 * math.log(ITEM_COUNT)
    log_forget = jax.nn.log_sigmoid(gate_pre[:, 1, :] + forget_bias) + forget_shift
    mem_blocks = ITEM_COUNT // BLK

    def blocks(array):
        return array.astype(jnp.float32).reshape(mem_blocks, BLK, CELL_SUBSPACES, HD).transpose(0, 2, 1, 3)

    def gate_blocks(array):
        return array.reshape(mem_blocks, BLK, CELL_SUBSPACES).transpose(0, 2, 1)
    initial = (jnp.zeros((CELL_SUBSPACES, HD, HD), jnp.float32), jnp.zeros((CELL_SUBSPACES, HD), jnp.float32), jnp.full((CELL_SUBSPACES,), MASKED, jnp.float32))
    inputs = (blocks(mem_query), blocks(mem_key) * HD ** (-0.5), blocks(mem_value), gate_blocks(log_in), gate_blocks(log_forget))
    _, recall = lax.scan(block_step, initial, inputs)
    recall = recall.transpose(0, 2, 1, 3).reshape(ITEM_COUNT, CELL_SUBSPACES * HD)
    mem_out = (recall * jax.nn.sigmoid(mem_gate.astype(jnp.float32))).astype(jnp.bfloat16)
    joined = jnp.concatenate([attn_out, mem_out], axis=1)
    mixed = jnp.dot(joined, w_out, preferred_element_type=jnp.float32).astype(jnp.bfloat16)
    return (mixed, log_total)
```

```python
import math

import jax
import jax.numpy as jnp
from jax import lax
from jax.sharding import PartitionSpec as P

HD = 64
WINDOW = 128


EPSILON = 1e-06
MASKED = -1e30


def passed_along(block, axis, distance):
    devices = range(lax.axis_size(axis))
    route = [(i - distance, i) for i in devices if i - distance in devices]
    return lax.ppermute(block, axis, route)


def shifted(block, axis, distance):
    n = lax.axis_size(axis)
    return lax.ppermute(block, axis, [(i, (i + distance) % n) for i in range(n)])


def flipped(block, axis):
    return lax.ppermute(block, axis, [(i, i ^ 1) for i in range(lax.axis_size(axis))])


def spread(shard, axis):
    n = lax.axis_size(axis)
    place = lax.axis_index(axis)
    pieces = []
    for k in range(n // 2):
        mine = shard if k == 0 else shifted(shard, axis, 2 * k)
        pieces.append(((place - 2 * k) % n, mine))
        pieces.append(((lax.bitwise_xor(place, 1) - 2 * k) % n, flipped(mine, axis)))
    return pieces


def product(rows, pieces):
    total = None
    for owner, piece in pieces:
        depth = piece.shape[0]
        columns = lax.dynamic_slice_in_dim(rows, owner * depth, depth, 1)
        part = jnp.dot(columns, piece, preferred_element_type=jnp.float32)
        total = part if total is None else total + part
    return total


def normalize(tokens, norm_gain):
    values = tokens.astype(jnp.float32)
    rescale = lax.rsqrt(jnp.mean(values * values, axis=-1, keepdims=True) + EPSILON)
    return (values * rescale * norm_gain).astype(jnp.bfloat16)


def attend(query, key_rows, value_rows, sinks):
    row_count = query.shape[0]
    kv_local = key_rows.shape[1] // HD
    group_size = query.shape[1] // HD // kv_local
    block_count = row_count // WINDOW
    rim_key, rim_value = passed_along(
        (key_rows[row_count - WINDOW :], value_rows[row_count - WINDOW :]), "sp", 1
    )
    padded_keys = jnp.concatenate([rim_key, key_rows], axis=0).reshape(
        block_count + 1, WINDOW, kv_local, HD
    )
    padded_values = jnp.concatenate([rim_value, value_rows], axis=0).reshape(
        block_count + 1, WINDOW, kv_local, HD
    )
    key_window = jnp.concatenate([padded_keys[:-1], padded_keys[1:]], axis=1)
    value_window = jnp.concatenate([padded_values[:-1], padded_values[1:]], axis=1)
    q_blocks = query.reshape(block_count, WINDOW, kv_local, group_size, HD)
    scores = jnp.einsum(
        "nqhgd,nkhd->nhgqk", q_blocks, key_window, preferred_element_type=jnp.float32
    ) * HD ** (-0.5)
    query_index = lax.broadcasted_iota(jnp.int32, (WINDOW, 2 * WINDOW), 0)
    key_index = lax.broadcasted_iota(jnp.int32, (WINDOW, 2 * WINDOW), 1)
    distance = query_index - key_index + WINDOW
    in_band = (distance >= 0) & (distance < WINDOW)
    block_index = lax.broadcasted_iota(jnp.int32, (block_count, WINDOW, 2 * WINDOW), 0)
    key_position = (
        lax.axis_index("sp") * row_count + block_index * WINDOW - WINDOW + key_index[None]
    )
    allowed = (in_band[None] & (key_position >= 0))[:, None, None]
    scores = jnp.where(allowed, scores, MASKED)
    sink_logit = sinks.reshape(1, kv_local, group_size, 1, 1)
    ceiling = jnp.maximum(jnp.max(scores, axis=-1, keepdims=True), sink_logit)
    weights = jnp.exp(scores - ceiling)
    partition = jnp.exp(sink_logit - ceiling) + jnp.sum(weights, axis=-1, keepdims=True)
    log_total = (
        (ceiling + jnp.log(partition))[..., 0]
        .transpose(0, 3, 1, 2)
        .reshape(row_count, kv_local * group_size)
    )
    probs = (weights / partition).astype(jnp.bfloat16)
    head_out = jnp.einsum(
        "nhgqk,nkhd->nqhgd", probs, value_window, preferred_element_type=jnp.float32
    )
    return (head_out.astype(jnp.bfloat16).reshape(row_count, kv_local * group_size * HD), log_total)


def dot16(spec, left, right):
    return jnp.einsum(
        spec,
        left.astype(jnp.bfloat16),
        right.astype(jnp.bfloat16),
        preferred_element_type=jnp.float32,
    )


def memory(mem_query, mem_key, mem_value, mem_gate, gate_pre, forget_bias, forget_shift):
    row_count = mem_query.shape[0]
    head_count = forget_bias.shape[0]
    sequence_total = row_count * lax.axis_size("sp")

    def heads(array):
        return array.reshape(row_count, head_count, HD).transpose(1, 0, 2)

    log_in = (gate_pre[:, 0, :] - 0.5 * math.log(sequence_total)).T
    log_forget = (jax.nn.log_sigmoid(gate_pre[:, 1, :] + forget_bias) + forget_shift).T
    cumulative = jnp.cumsum(log_forget, axis=-1)
    passed = cumulative[:, -1]
    query = heads(mem_query)
    key = heads(mem_key) * jnp.asarray(HD ** (-0.5), mem_key.dtype)
    value = heads(mem_value)

    decays = passed[:, None] - cumulative + log_in
    level = jnp.max(decays, axis=-1)
    weights = jnp.exp(decays - level[:, None])
    state = dot16("hsv,hsk->hvk", value.astype(jnp.float32) * weights[:, :, None], key)
    normal = jnp.sum(weights[:, :, None] * key.astype(jnp.float32), axis=1)
    scalars = jnp.concatenate(
        [passed[:, None, None], level[:, None, None], jnp.zeros((head_count, 1, HD - 2), jnp.float32)],
        axis=2,
    )
    packed = jnp.concatenate([state, normal[:, None, :], scalars], axis=1)
    gathered = lax.all_gather(packed, "sp")
    place = lax.axis_index("sp")
    passed_all, level_all = gathered[:, :, HD + 1, 0], gathered[:, :, HD + 1, 1]
    device = jnp.arange(passed_all.shape[0])[:, None]
    earlier = device < place
    through = jnp.cumsum(jnp.where(earlier, passed_all, 0.0), axis=0)
    entry_log = jnp.where(earlier, through[-1:] - through + level_all, MASKED)
    stabilizer = jnp.max(entry_log, axis=0)
    entry_weight = jnp.where(earlier, jnp.exp(entry_log - stabilizer[None]), 0.0)
    entering = jnp.sum(entry_weight[:, :, None, None] * gathered[:, :, : HD + 1, :], axis=0)

    causal = lax.broadcasted_iota(jnp.int32, (row_count, row_count), 0) >= lax.broadcasted_iota(
        jnp.int32, (row_count, row_count), 1
    )
    log_weight = jnp.where(
        causal[None], cumulative[:, :, None] + (log_in - cumulative)[:, None, :], MASKED
    )
    row_level = jnp.maximum(cumulative + stabilizer[:, None], jnp.max(log_weight, axis=-1))
    carried_part = jnp.exp(cumulative + stabilizer[:, None] - row_level)
    affinity = dot16("htd,hsd->hts", query, key) * jnp.exp(log_weight - row_level[:, :, None])
    carried = dot16("hvk,htk->htv", entering, query)
    numerator = carried_part[:, :, None] * carried[:, :, :HD] + dot16(
        "hts,hsv->htv", affinity, value
    )
    denominator = carried_part * carried[:, :, HD] + jnp.sum(affinity, axis=-1)
    recall = numerator / jnp.maximum(jnp.abs(denominator), jnp.exp(-row_level))[:, :, None]
    recall = recall.transpose(1, 0, 2).reshape(row_count, head_count * HD)
    return (recall * jax.nn.sigmoid(mem_gate.astype(jnp.float32))).astype(jnp.bfloat16)


def shards(
    tokens,
    norm_gain,
    w_query,
    w_key,
    w_value,
    w_mem_query,
    w_mem_key,
    w_mem_value,
    w_mem_gate,
    w_gates,
    sinks,
    forget_bias,
    forget_shift,
    w_out,
):
    normed = normalize(tokens, norm_gain)
    token_rows = lax.all_gather(normed, "tp", axis=0, tiled=True)
    row_count = token_rows.shape[0]
    head_count = forget_bias.shape[0]
    gate_columns = lax.dynamic_slice_in_dim(
        w_gates, lax.axis_index("tp") * head_count, head_count, 2
    ).reshape(w_gates.shape[0], 2 * head_count)
    gate_pre = jnp.dot(token_rows, gate_columns, preferred_element_type=jnp.float32).reshape(
        row_count, 2, head_count
    )
    mem_shard = jnp.concatenate([w_mem_query, w_mem_key, w_mem_value, w_mem_gate], axis=1)
    attn_shard = jnp.concatenate([w_query, w_key, w_value], axis=1)
    mem_pieces = spread(mem_shard, "sp")
    attn_pieces = spread(attn_shard, "sp")
    out_pieces = spread(w_out, "sp")
    mem_all = product(token_rows, mem_pieces).astype(jnp.bfloat16)
    attn_all = product(token_rows, attn_pieces).astype(jnp.bfloat16)
    mem_parts = jnp.split(mem_all, 4, axis=1)
    mem_out = memory(
        mem_parts[0], mem_parts[1], mem_parts[2], mem_parts[3], gate_pre, forget_bias, forget_shift
    )
    q_cols, k_cols = w_query.shape[1], w_key.shape[1]
    attn_out, log_total = attend(
        attn_all[:, :q_cols],
        attn_all[:, q_cols : q_cols + k_cols],
        attn_all[:, q_cols + k_cols :],
        sinks,
    )
    head_attn, head_mem = (
        lax.all_gather(attn_out, "tp", axis=1, tiled=True),
        lax.all_gather(mem_out, "tp", axis=1, tiled=True),
    )
    joined = jnp.concatenate([head_attn, head_mem], axis=1)
    mixed = product(joined, out_pieces)
    return (mixed.astype(jnp.bfloat16), log_total)


def solution(mesh):
    placed = (
        P(("sp", "tp"), None),
        P(),
        P("sp", "tp"),
        P("sp", "tp"),
        P("sp", "tp"),
        P("sp", "tp"),
        P("sp", "tp"),
        P("sp", "tp"),
        P("sp", "tp"),
        P(),
        P("tp"),
        P("tp"),
        P("sp", "tp"),
        P("sp", "tp"),
    )
    return jax.shard_map(
        shards,
        mesh=mesh,
        in_specs=placed,
        out_specs=(P("sp", "tp"), P("sp", "tp")),
        check_vma=False,
    )
```

```python
import functools
import math

import jax
import jax.numpy as jnp
from jax import lax
from jax.experimental import pallas as pl
from jax.experimental.pallas import tpu as pltpu
from jax.sharding import PartitionSpec as P

HD = 64
WINDOW = 128


EPSILON = 1e-06
MASKED = -1e30


def passed_along(block, axis, distance):
    devices = range(lax.axis_size(axis))
    route = [(i - distance, i) for i in devices if i - distance in devices]
    return lax.ppermute(block, axis, route)


def line_gather_kernel(chunks, count, *refs):
    shards, wholes = refs[:count], refs[count : 2 * count]
    own_sems, send_sems, recv_sems = refs[2 * count :]
    line = lax.axis_size("sp") // 2
    me = lax.axis_index("sp")
    z = me // 2
    y = me % 2
    twin = me + 1 - 2 * y
    targets = (me + 2, me - 2, twin)
    can_up, can_down = z < line - 1, z > 0

    barrier = pltpu.get_barrier_semaphore()

    def greet(target):
        pl.semaphore_signal(
            barrier, inc=1, device_id={"sp": target}, device_id_type=pl.DeviceIdType.MESH
        )

    greet(twin)
    pl.when(can_up)(lambda: greet(me + 2))
    pl.when(can_down)(lambda: greet(me - 2))
    inside = jnp.logical_and(can_up, can_down)
    pl.when(inside)(lambda: pl.semaphore_wait(barrier, 3))
    pl.when(jnp.logical_not(inside))(lambda: pl.semaphore_wait(barrier, 2))

    def copy(c, owner, way, own=False):
        which, first, rows, _ = chunks[c]
        depth = shards[which].shape[0]
        start = pl.multiple_of(owner * depth + first, math.gcd(math.gcd(depth, first), rows))
        place = wholes[which].at[pl.ds(start, rows), :]
        return pltpu.make_async_remote_copy(
            src_ref=shards[which].at[pl.ds(first, rows), :] if own else place,
            dst_ref=place,
            send_sem=send_sems.at[c, owner, way],
            recv_sem=recv_sems.at[c, owner],
            device_id={"sp": targets[way]},
            device_id_type=pl.DeviceIdType.MESH,
        )

    def outgoing(act):
        every = range(len(chunks))
        for c in every:
            act(c, me, 2, True, False)
            pl.when(can_up)(functools.partial(act, c, me, 0, True, False))
            pl.when(can_down)(functools.partial(act, c, me, 1, True, False))
        for c in every:
            if chunks[c][3]:
                arrive(act, c, twin)
                pl.when(can_up)(functools.partial(act, c, twin, 0, False, False))
                pl.when(can_down)(functools.partial(act, c, twin, 1, False, False))

        def step(t, nothing):
            for c in every:
                swap_first = chunks[c][3]
                for way, origin, there, further in (
                    (0, z - t, z - t >= 0, can_up),
                    (1, z + t, z + t < line, can_down),
                ):

                    def landed(way=way, origin=origin, further=further, c=c):
                        for side in (y, 1 - y) if swap_first else (y,):
                            owner = origin * 2 + side
                            arrive(act, c, owner)
                            pl.when(further)(functools.partial(act, c, owner, way, False, False))
                            if not swap_first:
                                act(c, owner, 2, False, False)

                    pl.when(there)(landed)
            return nothing

        lax.fori_loop(1, line, step, 0)

    def arrive(act, c, owner):
        if act is start:
            copy(c, owner, 2).wait_recv()

    def start(c, owner, way, own, _):
        copy(c, owner, way, own).start()

    def sent(c, owner, way, own, _):
        copy(c, owner, way, own).wait_send()

    def keep(which):
        depth = shards[which].shape[0]
        begin = pl.multiple_of(me * depth, depth)
        return pltpu.make_async_copy(
            shards[which], wholes[which].at[pl.ds(begin, depth), :], own_sems.at[which]
        )

    outgoing(start)
    for which in range(count):
        keep(which).start()

    def swapped(origin, nothing):
        for c in range(len(chunks)):
            if not chunks[c][3]:
                copy(c, origin * 2 + 1 - y, 2).wait_recv()
        return nothing

    lax.fori_loop(0, line, swapped, 0)
    outgoing(sent)
    for which in range(count):
        keep(which).wait()


def line_gather(shards, cuts, swap_first, collective_id):
    n = lax.axis_size("sp")
    chunks = []
    for which, (shard, cut) in enumerate(zip(shards, cuts)):
        rows = shard.shape[0] // cut
        chunks += [(which, i * rows, rows, which in swap_first) for i in range(cut)]
    count = len(shards)
    sent = sum(shard.size for shard in shards) * 2 * (n - 1)
    return pl.pallas_call(
        functools.partial(line_gather_kernel, chunks, count),
        out_shape=[
            jax.ShapeDtypeStruct((n * shard.shape[0], shard.shape[1]), shard.dtype)
            for shard in shards
        ],
        in_specs=[pl.BlockSpec(memory_space=pl.ANY)] * count,
        out_specs=[pl.BlockSpec(memory_space=pl.ANY)] * count,
        scratch_shapes=[
            pltpu.SemaphoreType.DMA((count,)),
            pltpu.SemaphoreType.DMA((len(chunks), n, 3)),
            pltpu.SemaphoreType.DMA((len(chunks), n)),
        ],
        compiler_params=pltpu.CompilerParams(
            collective_id=collective_id, has_side_effects=True
        ),
        cost_estimate=pl.CostEstimate(flops=0, bytes_accessed=20 * sent, transcendentals=0),
    )(*shards)


def normalize(tokens, norm_gain):
    values = tokens.astype(jnp.float32)
    rescale = lax.rsqrt(jnp.mean(values * values, axis=-1, keepdims=True) + EPSILON)
    return (values * rescale * norm_gain).astype(jnp.bfloat16)


def attend(query, key_rows, value_rows, sinks):
    row_count = query.shape[0]
    kv_local = key_rows.shape[1] // HD
    group_size = query.shape[1] // HD // kv_local
    block_count = row_count // WINDOW
    rim_key, rim_value = passed_along(
        (key_rows[row_count - WINDOW :], value_rows[row_count - WINDOW :]), "sp", 1
    )
    padded_keys = jnp.concatenate([rim_key, key_rows], axis=0).reshape(
        block_count + 1, WINDOW, kv_local, HD
    )
    padded_values = jnp.concatenate([rim_value, value_rows], axis=0).reshape(
        block_count + 1, WINDOW, kv_local, HD
    )
    key_window = jnp.concatenate([padded_keys[:-1], padded_keys[1:]], axis=1)
    value_window = jnp.concatenate([padded_values[:-1], padded_values[1:]], axis=1)
    q_blocks = query.reshape(block_count, WINDOW, kv_local, group_size, HD)
    scores = jnp.einsum(
        "nqhgd,nkhd->nhgqk", q_blocks, key_window, preferred_element_type=jnp.float32
    ) * HD ** (-0.5)
    query_index = lax.broadcasted_iota(jnp.int32, (WINDOW, 2 * WINDOW), 0)
    key_index = lax.broadcasted_iota(jnp.int32, (WINDOW, 2 * WINDOW), 1)
    distance = query_index - key_index + WINDOW
    in_band = (distance >= 0) & (distance < WINDOW)
    block_index = lax.broadcasted_iota(jnp.int32, (block_count, WINDOW, 2 * WINDOW), 0)
    key_position = (
        lax.axis_index("sp") * row_count + block_index * WINDOW - WINDOW + key_index[None]
    )
    allowed = (in_band[None] & (key_position >= 0))[:, None, None]
    scores = jnp.where(allowed, scores, MASKED)
    sink_logit = sinks.reshape(1, kv_local, group_size, 1, 1)
    ceiling = jnp.maximum(jnp.max(scores, axis=-1, keepdims=True), sink_logit)
    weights = jnp.exp(scores - ceiling)
    partition = jnp.exp(sink_logit - ceiling) + jnp.sum(weights, axis=-1, keepdims=True)
    log_total = (
        (ceiling + jnp.log(partition))[..., 0]
        .transpose(0, 3, 1, 2)
        .reshape(row_count, kv_local * group_size)
    )
    probs = (weights / partition).astype(jnp.bfloat16)
    head_out = jnp.einsum(
        "nhgqk,nkhd->nqhgd", probs, value_window, preferred_element_type=jnp.float32
    )
    return (head_out.astype(jnp.bfloat16).reshape(row_count, kv_local * group_size * HD), log_total)


def dot16(spec, left, right):
    return jnp.einsum(
        spec,
        left.astype(jnp.bfloat16),
        right.astype(jnp.bfloat16),
        preferred_element_type=jnp.float32,
    )


def memory(mem_query, mem_key, mem_value, mem_gate, gate_pre, forget_bias, forget_shift):
    row_count = mem_query.shape[0]
    head_count = forget_bias.shape[0]
    sequence_total = row_count * lax.axis_size("sp")

    def heads(array):
        return array.reshape(row_count, head_count, HD).transpose(1, 0, 2)

    log_in = (gate_pre[:, 0, :] - 0.5 * math.log(sequence_total)).T
    log_forget = (jax.nn.log_sigmoid(gate_pre[:, 1, :] + forget_bias) + forget_shift).T
    cumulative = jnp.cumsum(log_forget, axis=-1)
    passed = cumulative[:, -1]
    query = heads(mem_query)
    key = heads(mem_key) * jnp.asarray(HD ** (-0.5), mem_key.dtype)
    value = heads(mem_value)

    decays = passed[:, None] - cumulative + log_in
    level = jnp.max(decays, axis=-1)
    weights = jnp.exp(decays - level[:, None])
    state = dot16("hsv,hsk->hvk", value.astype(jnp.float32) * weights[:, :, None], key)
    normal = jnp.sum(weights[:, :, None] * key.astype(jnp.float32), axis=1)
    scalars = jnp.concatenate(
        [passed[:, None, None], level[:, None, None], jnp.zeros((head_count, 1, HD - 2), jnp.float32)],
        axis=2,
    )
    packed = jnp.concatenate([state, normal[:, None, :], scalars], axis=1)
    n = lax.axis_size("sp")
    gathered = jnp.stack([passed_along(packed, "sp", k) for k in range(1, n)])
    passed_all, level_all = gathered[:, :, HD + 1, 0], gathered[:, :, HD + 1, 1]
    earlier = jnp.arange(1, n)[:, None] <= lax.axis_index("sp")
    between = jnp.cumsum(passed_all, axis=0) - passed_all
    entry_log = jnp.where(earlier, between + level_all, MASKED)
    stabilizer = jnp.max(entry_log, axis=0)
    entry_weight = jnp.where(earlier, jnp.exp(entry_log - stabilizer[None]), 0.0)
    entering = jnp.sum(entry_weight[:, :, None, None] * gathered[:, :, : HD + 1, :], axis=0)

    causal = lax.broadcasted_iota(jnp.int32, (row_count, row_count), 0) >= lax.broadcasted_iota(
        jnp.int32, (row_count, row_count), 1
    )
    log_weight = jnp.where(
        causal[None], cumulative[:, :, None] + (log_in - cumulative)[:, None, :], MASKED
    )
    row_level = jnp.maximum(cumulative + stabilizer[:, None], jnp.max(log_weight, axis=-1))
    carried_part = jnp.exp(cumulative + stabilizer[:, None] - row_level)
    affinity = dot16("htd,hsd->hts", query, key) * jnp.exp(log_weight - row_level[:, :, None])
    carried = dot16("hvk,htk->htv", entering, query)
    numerator = carried_part[:, :, None] * carried[:, :, :HD] + dot16(
        "hts,hsv->htv", affinity, value
    )
    denominator = carried_part * carried[:, :, HD] + jnp.sum(affinity, axis=-1)
    recall = numerator / jnp.maximum(jnp.abs(denominator), jnp.exp(-row_level))[:, :, None]
    recall = recall.transpose(1, 0, 2).reshape(row_count, head_count * HD)
    return (recall * jax.nn.sigmoid(mem_gate.astype(jnp.float32))).astype(jnp.bfloat16)


def shards(
    tokens,
    norm_gain,
    w_query,
    w_key,
    w_value,
    w_mem_query,
    w_mem_key,
    w_mem_value,
    w_mem_gate,
    w_gates,
    sinks,
    forget_bias,
    forget_shift,
    w_out,
):
    normed, w_key = lax.optimization_barrier((normalize(tokens, norm_gain), w_key))
    token_rows = lax.all_gather(normed, "tp", axis=0, tiled=True)
    row_count = token_rows.shape[0]
    head_count = forget_bias.shape[0]
    gate_columns = lax.dynamic_slice_in_dim(
        w_gates, lax.axis_index("tp") * head_count, head_count, 2
    ).reshape(w_gates.shape[0], 2 * head_count)
    gate_pre = jnp.dot(token_rows, gate_columns, preferred_element_type=jnp.float32).reshape(
        row_count, 2, head_count
    )
    shard = jnp.concatenate(
        [w_mem_query, w_mem_key, w_mem_value, w_mem_gate, w_query, w_key, w_value], axis=1
    )
    full = line_gather((shard,), (2,), (), 0)[0]
    out_rows = lax.all_gather(w_out, "sp", axis=0, tiled=True)
    projected = jnp.dot(token_rows, full, preferred_element_type=jnp.float32).astype(jnp.bfloat16)
    mem_cols, q_cols, k_cols = w_mem_query.shape[1], w_query.shape[1], w_key.shape[1]
    mem_parts = jnp.split(projected[:, : 4 * mem_cols], 4, axis=1)
    attn_all = projected[:, 4 * mem_cols :]
    mem_out = memory(
        mem_parts[0], mem_parts[1], mem_parts[2], mem_parts[3], gate_pre, forget_bias, forget_shift
    )
    attn_out, log_total = attend(
        attn_all[:, :q_cols],
        attn_all[:, q_cols : q_cols + k_cols],
        attn_all[:, q_cols + k_cols :],
        sinks,
    )
    head_attn, head_mem = (
        lax.all_gather(attn_out, "tp", axis=1, tiled=True),
        lax.all_gather(mem_out, "tp", axis=1, tiled=True),
    )
    joined = jnp.concatenate([head_attn, head_mem], axis=1)
    mixed = jnp.dot(joined, out_rows, preferred_element_type=jnp.float32)
    return (mixed.astype(jnp.bfloat16), log_total)


def solution(mesh):
    placed = (
        P(("sp", "tp"), None),
        P(),
        P("sp", "tp"),
        P("sp", "tp"),
        P("sp", "tp"),
        P("sp", "tp"),
        P("sp", "tp"),
        P("sp", "tp"),
        P("sp", "tp"),
        P(),
        P("tp"),
        P("tp"),
        P("sp", "tp"),
        P("sp", "tp"),
    )
    return jax.shard_map(
        shards,
        mesh=mesh,
        in_specs=placed,
        out_specs=(P("sp", "tp"), P("sp", "tp")),
        check_vma=False,
    )
```
